32 devices in a mesh: sp: 8 (over z, y), tp: 4 (over x, core).
Axes of the slice: x: 2, y: 2, z: 4, core: 2. Of those that a mesh axis runs over, the one named last changes fastest.
Arguments:
- cotangent: bfloat16 [1024, 2048], P('sp', 'tp'), may hold values from -6 to 6
- mixer_out: bfloat16 [1024, 2048], P('sp', 'tp'), may hold values from -6 to 6
- route_ids: int32 [1024, 2], P('sp'), may hold values from 0 to 7, all different within a row; in each aligned block of 128 rows (0 to 127, 128 to 255, ...) at most 64 rows name the same one
- route_weights: float32 [1024, 2], P('sp'), may hold values from 0.2 to 1
- conv_out: bfloat16 [1024, 2048], P('sp', 'tp'), may hold values from -6 to 6
- recur_gate: bfloat16 [1024, 2048], P('sp', 'tp'), may hold values from 0.007 to 1
- input_gate: bfloat16 [1024, 2048], P('sp', 'tp'), may hold values from 0.099609375 to 0.8984375
- gate_pre: bfloat16 [1024, 2048], P('sp', 'tp'), may hold values from -6 to 6
- states_before: bfloat16 [1024, 2048], P('sp', 'tp'), may hold values from -4 to 4
- decay_rate: float32 [2048], P('tp'), may hold values from 4e-07 to 0.008
- out_proj: bfloat16 [2048, 2048], P(None, 'tp'), may hold values from -0.125 to 0.125
- recur_map: bfloat16 [4, 512, 512], P('tp'), may hold values from -0.25 to 0.25
- input_map: bfloat16 [4, 512, 512], P('tp'), may hold values from -0.25 to 0.25
- expert_gate: bfloat16 [8, 2048, 1024], P('sp', None, 'tp'), may hold values from -0.125 to 0.125
- expert_up: bfloat16 [8, 2048, 1024], P('sp', None, 'tp'), may hold values from -0.125 to 0.125
- expert_down: bfloat16 [8, 1024, 2048], P('sp', 'tp'), may hold values from -0.1875 to 0.1875
Outputs:
- grad_expert_gate: bfloat16 [8, 2048, 1024], P('sp', None, 'tp')
- grad_expert_up: bfloat16 [8, 2048, 1024], P('sp', None, 'tp')
- grad_expert_down: bfloat16 [8, 1024, 2048], P('sp', 'tp')
- grad_out_proj: float32 [2048, 2048], P('sp', 'tp')
- grad_conv: bfloat16 [1024, 2048], P('sp', 'tp')
- grad_gate_pre: bfloat16 [1024, 2048], P('sp', 'tp')
The draws below stay inside these ranges and needn't reach their ends.
Inputs may be any that keep to these rules, and one draw needn't show every extreme that they name: `route_ids`: the two experts of a token differ. In every aligned block of 128 tokens no expert is named by more than 64 routes, and in some block some expert by exactly 64.
All inputs are finite; a program needn't handle non-finite values.
Results may differ from the reference program's by a relative error of at most 0.0093.
Values may be sent and summed in bfloat16 or wider, within the bound.
No kernel may reach another device: no remote copies, remote signals or barrier semaphores. Data moves between devices by JAX's collectives and lax.ppermute only.
A program may use at most 64 MiB of HBM per device.

```python
import math
import jax
import jax.numpy as jnp
import numpy as np
from jax import lax

D = 2048
LRU = 2048
BLOCKS = 4
BLOCK_W = 512
FF = 1024
TOK_DEV = 128
TOKENS = 1024
EXPERTS = 8
CAP = 64
N_SP = 8


def draw_recur_gate(key, part):
    key_one, key_two = jax.random.split(key)
    span_count = TOKENS // 128
    base_gate = jax.random.uniform(key_one, (TOKENS, LRU), jnp.float32, 0.5, 1.0)
    factor = jnp.exp(jax.random.uniform(key_two, (span_count, 1, 1), jnp.float32, math.log(0.15), 0.0))
    return (base_gate.reshape(span_count, 128, LRU) * factor).reshape(TOKENS, LRU).astype(jnp.bfloat16)


def draw_decay_rate(key, part):
    key_one, key_two, key_three = jax.random.split(key, 3)
    fast_share = 0.5
    fast_mask = jax.random.bernoulli(key_one, fast_share, (LRU,))
    slow_rate = jnp.exp(jax.random.uniform(key_two, (LRU,), jnp.float32, math.log(0.03), math.log(0.25))) / TOKENS
    fast_rate = jnp.exp(jax.random.uniform(key_three, (LRU,), jnp.float32, math.log(0.002), math.log(0.008)))
    return jnp.where(fast_mask, fast_rate, slow_rate).astype(jnp.float32)


def with_spikes(entries, own_key, source, target, shards_of, factor):
    owner, partner = [(jnp.arange(entries.shape[axis_at]) // (entries.shape[axis_at] // shards_of)).reshape([-1 if axis == axis_at else 1 for axis in range(entries.ndim)]) for axis_at in (source, target)]
    chosen = jax.random.permutation(own_key, shards_of)[partner]
    strong = (owner == chosen) | (owner == (partner + shards_of // 2) % shards_of)
    return jnp.where(strong, factor * entries, entries)


def steps_of(own_key, extent, cuts, smallest, largest):
    level, own = 1.0, jax.random.fold_in(own_key, 6)
    for position, parts in cuts:
        steps = jnp.exp(jax.random.uniform(jax.random.fold_in(own, position), (parts,), jnp.float32, smallest / len(cuts), largest / len(cuts)))
        level = level * jnp.repeat(steps, extent[position] // parts).reshape([-1 if axis == position else 1 for axis in range(len(extent))])
    return level


def shared_out(rng, own, number, rows, number_of, top, reach, skew):
    order = jax.random.permutation(rng, number_of)
    packed, ordinary = load_shares(number_of, rows * top, reach, skew, True), load_shares(number_of, rows * top, reach, skew, False)
    places = jnp.arange(number_of)

    def named(tallies, turn):
        used = int((tallies > 0).sum())
        fixed = max(1, used // 4)
        moved = fixed + (places - fixed + turn * (used - fixed)) % max(1, number_of - fixed)
        return jnp.zeros((number_of,), jnp.int32).at[order[jnp.where(places < fixed, places, moved)]].set(jnp.asarray(tallies, jnp.int32))

    tallies = jnp.where(number % 4 == 0, named(packed, number // 4), named(ordinary, number - number // 4 - 1))
    mixed = jax.random.permutation(jax.random.fold_in(own, 3), number_of)
    donor, taker = mixed[0:number_of // 2 * 2:2], mixed[1:number_of // 2 * 2:2]
    margin = jnp.minimum(tallies[donor] - 1, reach - tallies[taker]) // 2
    margin = jnp.where((donor == order[0]) | (taker == order[0]) | (tallies[taker] == 0), 0, jnp.maximum(margin, 0))
    moved = jax.random.randint(jax.random.fold_in(own, 4), (number_of // 2,), 0, 1 << 20) % (margin + 1)
    tallies = tallies.at[donor].add(-moved).at[taker].add(moved)
    items = jnp.searchsorted(jnp.cumsum(tallies), jnp.arange(rows * top), side="right").astype(jnp.int32)
    listing = items.reshape(top, rows).T
    listing = listing[jax.random.permutation(jax.random.fold_in(own, 1), rows)]
    turn = jax.random.randint(jax.random.fold_in(own, 2), (rows, 1), 0, top)
    return jnp.take_along_axis(listing, (jnp.arange(top)[None, :] + turn) % top, axis=1)


def load_shares(amount, total, limit, lean, full):
    loads = [(1 << 20) // math.isqrt(standing ** lean) + 1 for standing in range(1, amount + 1)]
    largest = limit if full else min(limit, max(-(-total // amount), total * loads[0] // sum(loads)))
    least = 1 if total - largest >= amount - 1 else 0
    given, rest = [largest] + [least] * (amount - 1), total - largest - least * (amount - 1)
    while rest > 0:
        free = [i for i in range(1, amount) if given[i] < largest] or [i for i in range(1, amount) if given[i] < limit]
        mass, left = sum([loads[i] for i in free]), rest
        for i in free:
            extra = min(limit - given[i], max(1, left * loads[i] // mass), rest)
            given[i] = given[i] + extra
            rest = rest - extra
    return np.array(given)


def scatter_about(stream_key, dims, deviation, reach, cuts=(), held_as=jnp.bfloat16):
    loudness = steps_of(stream_key, dims, cuts, -0.22, 0.18) if cuts else 1.0
    values = jax.random.normal(stream_key, dims, jnp.float32) * deviation * loudness
    return jnp.minimum(jnp.maximum(values, -reach), reach).astype(held_as)


def noise_with(own_key, dims, width, reach, shards, heavy, kind=jnp.bfloat16):
    array = width * jax.random.normal(own_key, dims, jnp.float32)
    if shards:
        array = array * steps_of(own_key, dims, shards, -0.22, 0.18)
    return jnp.clip(with_spikes(array, jax.random.fold_in(own_key, 3), *heavy), -reach, reach).astype(kind)


def setup_inputs(seed: int = 0) -> dict:
    key_list = jax.random.split(jax.random.key(seed), 17)
    cotangent = noise_with(key_list[0], (TOKENS, D), 1.0, 6.0, ((0, 8), (1, 4)), (0, 1, 8, 2.0))
    mixer_out = scatter_about(key_list[1], (TOKENS, D), 1.0, 6.0, ((0, 8), (1, 4)))
    route_ids_keys = jax.random.split(jax.random.fold_in(key_list[2], 1), TOKENS // TOK_DEV)
    route_ids_turns = jax.random.permutation(jax.random.fold_in(key_list[2], 3), TOKENS // TOK_DEV)
    route_ids = jax.vmap(lambda own, number: shared_out(jax.random.fold_in(key_list[2], 2), own, number, TOK_DEV, EXPERTS, 2, CAP, 2))(route_ids_keys, route_ids_turns).reshape((TOKENS, 2))
    route_weights = jnp.clip(0.2 + 0.8 * jax.random.uniform(key_list[3], (TOKENS, 2), jnp.float32) ** steps_of(key_list[3], (TOKENS, 2), ((0, 8),), -0.2, 0.2), 0.2, 1.0)
    conv_out = scatter_about(key_list[4], (TOKENS, LRU), 1.0, 6.0, ((0, 8), (1, 4)))
    recur_gate = draw_recur_gate(jax.random.fold_in(key_list[16], 71), 0)
    input_gate = jnp.clip(0.099609375 + 0.7988281 * jax.random.uniform(key_list[6], (TOKENS, LRU), jnp.float32) ** steps_of(key_list[6], (TOKENS, LRU), ((0, 8), (1, 4)), -0.2, 0.2), 0.099609375, 0.8984375).astype(jnp.bfloat16)
    gate_pre = scatter_about(key_list[7], (TOKENS, LRU), 1.0, 6.0, ((0, 8), (1, 4)))
    states_before = scatter_about(key_list[8], (TOKENS, LRU), 0.5, 4.0, ((0, 8), (1, 4)))
    decay_rate = draw_decay_rate(jax.random.fold_in(key_list[16], 71), 0)
    out_proj = scatter_about(key_list[10], (D, LRU), LRU ** -0.5, 0.125, ((1, 4),))
    recur_map = scatter_about(key_list[11], (BLOCKS, BLOCK_W, BLOCK_W), BLOCK_W ** -0.5, 0.25, ((0, 4),))
    input_map = scatter_about(key_list[12], (BLOCKS, BLOCK_W, BLOCK_W), BLOCK_W ** -0.5, 0.25, ((0, 4),))
    expert_gate = scatter_about(key_list[13], (EXPERTS, D, FF), D ** -0.5, 0.125, ((0, 8), (2, 4)))
    expert_up = scatter_about(key_list[14], (EXPERTS, D, FF), D ** -0.5, 0.125, ((0, 8), (2, 4)))
    expert_down = scatter_about(key_list[15], (EXPERTS, FF, D), FF ** -0.5, 0.1875, ((0, 8), (1, 4)))
    return dict(cotangent=cotangent, mixer_out=mixer_out, route_ids=route_ids, route_weights=route_weights, conv_out=conv_out, recur_gate=recur_gate, input_gate=input_gate, gate_pre=gate_pre, states_before=states_before, decay_rate=decay_rate, out_proj=out_proj, recur_map=recur_map, input_map=input_map, expert_gate=expert_gate, expert_up=expert_up, expert_down=expert_down)


def silu_parts(values):
    sig = jax.nn.sigmoid(values)
    return (values * sig, sig * (1.0 + values * (1.0 - sig)))

def route_slots(route_block):
    flat_ids = route_block.reshape(-1)
    onehot = (flat_ids[:, None] == jnp.arange(EXPERTS, dtype=jnp.int32)[None, :]).astype(jnp.int32)
    before = jnp.cumsum(onehot, axis=0) - onehot
    slot_rank = lax.optimization_barrier(jnp.sum(before * onehot, axis=1))
    return (flat_ids * CAP + slot_rank).astype(jnp.int32)

def link_steps(earlier, later):
    return (earlier[0] * later[0], later[0] * earlier[1] + later[1])

def reference(cotangent, mixer_out, route_ids, route_weights, conv_out, recur_gate, input_gate, gate_pre, states_before, decay_rate, out_proj, recur_map, input_map, expert_gate, expert_up, expert_down):
    slot_pos = jax.vmap(route_slots)(route_ids.reshape(N_SP, TOK_DEV, 2))
    expert_of = slot_pos // CAP
    slot_rank = slot_pos % CAP
    source = jnp.arange(N_SP, dtype=jnp.int32)[:, None]
    place = (expert_of * (N_SP * CAP) + source * CAP + slot_rank).astype(jnp.int32).reshape(-1)
    token_of = (source * TOK_DEV + jnp.arange(2 * TOK_DEV, dtype=jnp.int32)[None, :] // 2).astype(jnp.int32)
    table = jnp.full((EXPERTS * N_SP * CAP,), TOKENS, jnp.int32).at[place].set(token_of.reshape(-1))
    slot_weight = jnp.zeros((EXPERTS * N_SP * CAP,), jnp.float32).at[place].set(route_weights.astype(jnp.float32).reshape(-1))
    table = table.reshape(EXPERTS, N_SP * CAP)
    slot_weight = slot_weight.reshape(EXPERTS, N_SP * CAP)
    x_padded = jnp.concatenate([mixer_out, jnp.zeros((1, D), jnp.bfloat16)], axis=0)
    g_padded = jnp.concatenate([cotangent, jnp.zeros((1, D), jnp.bfloat16)], axis=0)

    def expert_step(routed_sum, inputs):
        row_index, weight, w_gate, w_up, w_down = inputs
        row_data = x_padded[row_index]
        routed_cot = (g_padded[row_index].astype(jnp.float32) * weight[:, None]).astype(jnp.bfloat16)
        pre_gate = jnp.dot(row_data, w_gate, preferred_element_type=jnp.float32)
        pre_up = jnp.dot(row_data, w_up, preferred_element_type=jnp.float32)
        gate_act, slope = silu_parts(pre_gate)
        active = (gate_act * pre_up).astype(jnp.bfloat16)
        d_active = jnp.dot(routed_cot, w_down.T, preferred_element_type=jnp.float32)
        grad_down = jnp.dot(active.T, routed_cot, preferred_element_type=jnp.float32).astype(jnp.bfloat16)
        d_gate = (d_active * pre_up * slope).astype(jnp.bfloat16)
        d_up = (d_active * gate_act).astype(jnp.bfloat16)
        grad_gate = jnp.dot(row_data.T, d_gate, preferred_element_type=jnp.float32).astype(jnp.bfloat16)
        grad_up = jnp.dot(row_data.T, d_up, preferred_element_type=jnp.float32).astype(jnp.bfloat16)
        route_grad = (jnp.dot(d_gate, w_gate.T, preferred_element_type=jnp.float32) + jnp.dot(d_up, w_up.T, preferred_element_type=jnp.float32)).astype(jnp.bfloat16)
        routed_sum = routed_sum.at[row_index].add(route_grad.astype(jnp.float32))
        return (routed_sum, (grad_gate, grad_up, grad_down))
    routed_sum, expert_grads = lax.scan(expert_step, jnp.zeros((TOKENS + 1, D), jnp.float32), (table, slot_weight, expert_gate, expert_up, expert_down))
    grad_expert_gate, grad_expert_up, grad_expert_down = expert_grads
    out_grad = (cotangent.astype(jnp.float32) + routed_sum[:TOKENS]).astype(jnp.bfloat16)
    rate = decay_rate.astype(jnp.float32)[None, :]
    recur_f = recur_gate.astype(jnp.float32)
    input_f = input_gate.astype(jnp.float32)
    conv_f = conv_out.astype(jnp.float32)
    before_f = states_before.astype(jnp.float32)
    log_decay = -8.0 * recur_f * rate
    decay_now = jnp.exp(log_decay)
    at_start = (jnp.arange(TOKENS, dtype=jnp.int32) == 0)[:, None]
    norm_factor = jnp.where(at_start, 1.0, jnp.sqrt(-jnp.expm1(2.0 * log_decay)))
    norm_slope = jnp.where(at_start, 0.0, -jnp.exp(2.0 * log_decay) / norm_factor)
    drive = input_f * conv_f
    state = decay_now * before_f + norm_factor * drive
    gate, gelu_back = jax.vjp(jax.nn.gelu, gate_pre.astype(jnp.float32))
    mixed = (state * gate).astype(jnp.bfloat16)
    d_mixed = jnp.dot(out_grad, out_proj, preferred_element_type=jnp.float32)
    grad_out_proj = jnp.dot(out_grad.T, mixed, preferred_element_type=jnp.float32)
    grad_gate_pre = gelu_back(d_mixed * state)[0].astype(jnp.bfloat16)
    decay_next = jnp.concatenate([decay_now[1:], jnp.ones((1, LRU), jnp.float32)], axis=0)
    _, state_grad = lax.associative_scan(link_steps, (decay_next, d_mixed * gate), axis=0, reverse=True)
    d_log = state_grad * (decay_now * before_f + norm_slope * drive)
    d_recur_pre = (d_log * (-8.0 * rate) * recur_f * (1.0 - recur_f)).astype(jnp.bfloat16)
    d_input_pre = (state_grad * norm_factor * conv_f * input_f * (1.0 - input_f)).astype(jnp.bfloat16)
    through_recur = jnp.einsum('tbj,bij->tbi', d_recur_pre.astype(jnp.float32).reshape(TOKENS, BLOCKS, BLOCK_W), recur_map.astype(jnp.float32))
    through_input = jnp.einsum('tbj,bij->tbi', d_input_pre.astype(jnp.float32).reshape(TOKENS, BLOCKS, BLOCK_W), input_map.astype(jnp.float32))
    grad_conv = (state_grad * norm_factor * input_f + (through_recur + through_input).reshape(TOKENS, LRU)).astype(jnp.bfloat16)
    return (grad_expert_gate, grad_expert_up, grad_expert_down, grad_out_proj, grad_conv, grad_gate_pre)
```

```python
import functools

import jax
import jax.numpy as jnp
from jax import lax
from jax.experimental import pallas as pl
from jax.experimental.pallas import tpu as pltpu
from jax.sharding import PartitionSpec as P

BF = jnp.bfloat16
F32 = jnp.float32
VM = pl.BlockSpec(memory_space=pltpu.VMEM)
SM = pl.BlockSpec(memory_space=pltpu.SMEM)


def hop(value, axis, bit):
    count = lax.axis_size(axis)
    return lax.ppermute(value, axis, [(i, i ^ bit) for i in range(count)])


def dot(left, right):
    return jnp.dot(left, right, preferred_element_type=F32)


def dot_nt(left, right):
    return lax.dot_general(left, right, (((1,), (1,)), ((), ())), preferred_element_type=F32)


def dot_tn(left, right):
    return lax.dot_general(left, right, (((0,), (0,)), ((), ())), preferred_element_type=F32)


def call(kernel, outs, ins, specs, flops):
    nbytes = sum(a.size * a.dtype.itemsize for a in list(outs) + list(ins))
    return pl.pallas_call(
        kernel,
        out_shape=list(outs),
        in_specs=specs,
        out_specs=[VM] * len(outs),
        cost_estimate=pl.CostEstimate(flops=flops, bytes_accessed=nbytes, transcendentals=0),
    )(*ins)


def struct(shape, dtype):
    return jax.ShapeDtypeStruct(shape, dtype)


def dispatch_kernel(n, cap, me_ref, ids_ref, w_ref, x_ref, g_ref, d_ref, *blocks):
    tok, feat = x_ref.shape
    ids = ids_ref[...] ^ me_ref[0]
    who = lax.broadcasted_iota(jnp.int32, (n, tok), 0)
    earlier = (
        lax.broadcasted_iota(jnp.int32, (tok, tok), 0)
        < lax.broadcasted_iota(jnp.int32, (tok, tok), 1)
    )
    earlier = jnp.where(earlier, 1.0, 0.0).astype(BF)
    one = [jnp.where(who == ids[k : k + 1, :], 1.0, 0.0) for k in range(2)]
    before = [dot(o.astype(BF), earlier) for o in one]
    before[1] = before[1] + jnp.sum(one[0], axis=1, keepdims=True)
    rank = [jnp.sum(b * o, axis=0, keepdims=True) for b, o in zip(before, one)]
    pos = [ids[k : k + 1, :] * cap + rank[k].astype(jnp.int32) for k in range(2)]
    slot = lax.broadcasted_iota(jnp.int32, (n * cap, tok), 0)
    hit = [slot == p for p in pos]
    weight = jnp.where(hit[0], w_ref[0:1, :], 0.0) + jnp.where(hit[1], w_ref[1:2, :], 0.0)
    weight = jnp.sum(weight, axis=1, keepdims=True)
    pick = jnp.where(hit[0] | hit[1], 1.0, 0.0).astype(BF)
    d_ref[...] = pick
    rows = dot(pick, x_ref[...]).astype(BF)
    cots = (dot(pick, g_ref[...]) * weight).astype(BF)
    for k, block in enumerate(blocks):
        block[:, :feat] = rows[k * cap : (k + 1) * cap]
        block[:, feat:] = cots[k * cap : (k + 1) * cap]


def expert_kernel(m, me_ref, *refs):
    parts, (wg_ref, wu_ref, wd_ref) = refs[:m], refs[m : m + 3]
    dg_ref, du_ref, act_ref, keep_ref, send_ref = refs[m + 3 :]
    feat = parts[0].shape[1] // 2

    def span(q):
        return pl.ds(pl.multiple_of((me_ref[0] ^ q) * feat, feat), feat)

    pre_gate = pre_up = d_active = 0.0
    for q in range(m):
        rows = parts[q][:, :feat]
        pre_gate += dot(rows, wg_ref[span(q), :])
        pre_up += dot(rows, wu_ref[span(q), :])
        d_active += dot_nt(parts[q][:, feat:], wd_ref[:, span(q)])
    sig = jax.nn.sigmoid(pre_gate)
    gate_act = pre_gate * sig
    act_ref[...] = (gate_act * pre_up).astype(BF)
    d_gate = (d_active * pre_up * sig * (1.0 + pre_gate * (1.0 - sig))).astype(BF)
    d_up = (d_active * gate_act).astype(BF)
    dg_ref[...] = d_gate
    du_ref[...] = d_up
    for q in range(m):
        part = dot_nt(d_gate, wg_ref[span(q), :]) + dot_nt(d_up, wu_ref[span(q), :])
        target = send_ref if q & 1 else keep_ref
        target[:, (q >> 1) * feat : ((q >> 1) + 1) * feat] = part.astype(BF)


def weight_kernel(m, chunks, me_ref, *refs):
    parts = [refs[h * m : (h + 1) * m] for h in range(chunks)]
    grads = refs[chunks * m : chunks * (m + 3)]
    gg_ref, gu_ref, gd_ref = refs[chunks * (m + 3) :]
    feat = parts[0][0].shape[1] // 2
    for q in range(m):
        span = pl.ds(pl.multiple_of((me_ref[0] ^ q) * feat, feat), feat)
        gate = up = down = 0.0
        for h in range(chunks):
            rows = parts[h][q][:, :feat]
            gate += dot_tn(rows, grads[3 * h][...])
            up += dot_tn(rows, grads[3 * h + 1][...])
            down += dot_tn(grads[3 * h + 2][...], parts[h][q][:, feat:])
        gg_ref[span, :] = gate.astype(BF)
        gu_ref[span, :] = up.astype(BF)
        gd_ref[:, span] = down.astype(BF)


def pair_sum_kernel(cap, keep_ref, got_ref, *outs):
    total = (keep_ref[...].astype(F32) + got_ref[...].astype(F32)).astype(BF)
    for k, out in enumerate(outs):
        out[...] = total[k * cap : (k + 1) * cap]


def combine_kernel(n, cap, d_ref, cot_ref, *refs):
    blocks, out_ref, held = refs[:n], refs[n], refs[n + 1]
    feat = cot_ref.shape[1]
    for k in range(n):
        held[k * cap : (k + 1) * cap, :] = blocks[k][...]
    total = dot_tn(d_ref[...], held[...])
    out_ref[:, :feat] = (total[:, :feat] + cot_ref[...].astype(F32)).astype(BF)
    out_ref[:, feat:] = total[:, feat:].astype(BF)


def recur_kernel(m, me_ref, og_ref, og_other_ref, op_ref, gate_ref, slope_ref, next_ref,
                 dgp_ref, local_ref, weight_ref):
    tok = og_ref.shape[0]
    feat = og_ref.shape[1] * 2 // m
    total = 0.0
    for q in range(m):
        span = pl.ds(pl.multiple_of((me_ref[0] ^ q) * feat, feat), feat)
        src = og_other_ref if q & 1 else og_ref
        total += dot(src[:, (q >> 1) * feat : ((q >> 1) + 1) * feat], op_ref[span, :])
    dgp_ref[...] = (total * slope_ref[...]).astype(BF)
    value = total * gate_ref[...]
    weight = next_ref[...]
    step = 1
    while step < tok:
        pad = jnp.zeros((step, value.shape[1]), F32)
        value = value + weight * jnp.concatenate([value[step:], pad], axis=0)
        weight = weight * jnp.concatenate([weight[step:], pad + 1.0], axis=0)
        step *= 2
    local_ref[...] = value
    weight_ref[...] = weight


def final_kernel(n, me_ref, local_ref, weight_ref, carry_ref, c1_ref, c2_ref, c3_ref, rm_ref, im_ref,
                 out_ref):
    incoming = jnp.zeros((1, local_ref.shape[1]), F32)
    for s in range(n - 1, 0, -1):
        longer = carry_ref[s, 1:2, :] + carry_ref[s, 0:1, :] * incoming
        incoming = jnp.where(s > me_ref[0], longer, incoming)
    grad = local_ref[...] + weight_ref[...] * incoming
    d_recur = (grad * c1_ref[...]).astype(BF)
    d_input = (grad * c2_ref[...]).astype(BF)
    groups, width = rm_ref.shape[0], rm_ref.shape[1]
    base = grad * c3_ref[...]
    for b in range(groups):
        cols = slice(b * width, (b + 1) * width)
        part = dot_nt(d_recur[:, cols], rm_ref[b]) + dot_nt(d_input[:, cols], im_ref[b])
        out_ref[:, cols] = (base[:, cols] + part).astype(BF)


def out_proj_kernel(n, me_ref, half_ref, own_ref, other_ref, mixed_ref, out_ref):
    rows = own_ref.shape[1]
    total = 0.0
    for s in range(n):
        for part, bit in ((own_ref, 0), (other_ref, 1)):
            at = ((me_ref[0] ^ s) * 2 + (half_ref[0] ^ bit)) * rows
            total += dot_tn(part[s], mixed_ref[pl.ds(pl.multiple_of(at, rows), rows), :])
    out_ref[...] = total


def body(
    cotangent,
    mixer_out,
    route_ids,
    route_weights,
    conv_out,
    recur_gate,
    input_gate,
    gate_pre,
    states_before,
    decay_rate,
    out_proj,
    recur_map,
    input_map,
    expert_gate,
    expert_up,
    expert_down,
):
    tok, feat = cotangent.shape
    n, m = lax.axis_size("sp"), lax.axis_size("tp")
    cap = 4 * tok // n
    sp, tp = lax.axis_index("sp").reshape(1), lax.axis_index("tp").reshape(1)
    slots = n * cap
    wg, wu, wd = expert_gate[0], expert_up[0], expert_down[0]
    hidden = wg.shape[1]
    channels = conv_out.shape[1]

    sent = call(
        functools.partial(dispatch_kernel, n, cap),
        [struct((slots, tok), BF)] + [struct((cap, 2 * feat), BF)] * n,
        [sp, route_ids.T, route_weights.T, mixer_out, cotangent],
        [SM, VM, VM, VM, VM],
        4 * slots * tok * feat,
    )
    pick, sent = sent[0], sent[1:]
    got = [sent[0]] + [hop(sent[k], "sp", k) for k in range(1, n)]

    rate = decay_rate[None, :]
    recur_f = recur_gate.astype(F32)
    input_f = input_gate.astype(F32)
    conv_f = conv_out.astype(F32)
    before_f = states_before.astype(F32)
    log_decay = -8.0 * recur_f * rate
    decay_now = jnp.exp(log_decay)
    position = lax.axis_index("sp") * tok + jnp.arange(tok, dtype=jnp.int32)
    at_start = (position == 0)[:, None]
    norm_factor = jnp.where(at_start, 1.0, jnp.sqrt(-jnp.expm1(2.0 * log_decay)))
    norm_slope = jnp.where(at_start, 0.0, -jnp.exp(2.0 * log_decay) / norm_factor)
    drive = input_f * conv_f
    kept = decay_now * before_f
    state = kept + norm_factor * drive
    gate, gelu_back = jax.vjp(jax.nn.gelu, gate_pre.astype(F32))
    slope = gelu_back(state)[0]
    mixed = (state * gate).astype(BF)
    decay_next = jnp.concatenate([decay_now[1:], jnp.ones((1, channels), F32)], axis=0)
    c1 = (kept + norm_slope * drive) * (-8.0 * rate) * recur_f * (1.0 - recur_f)
    c3 = norm_factor * input_f
    c2 = c3 * conv_f * (1.0 - input_f)

    all_mixed = mixed
    bit = n // 2
    pieces = {0: mixed}
    while bit:
        stacked = jnp.concatenate([pieces[k] for k in sorted(pieces)], axis=0)
        moved = hop(stacked, "sp", bit)
        order = sorted(pieces)
        for i, k in enumerate(order):
            pieces[k | bit] = moved[i * tok : (i + 1) * tok]
        bit //= 2
    all_mixed = jnp.concatenate([pieces[k] for k in range(n)], axis=0)

    chunks = [range(0, n // 2), range(n // 2, n)]
    parts, grads, back = [], [], [None] * n
    for chunk in chunks:
        here = {0: jnp.concatenate([got[k] for k in chunk], axis=0)}
        bit = m // 2
        while bit:
            for q in sorted(here):
                here[q | bit] = hop(here[q], "tp", bit)
            bit //= 2
        piece = [here[q] for q in range(m)]
        rows = len(chunk) * cap
        d_gate, d_up, active, keep, give = call(
            functools.partial(expert_kernel, m),
            [struct((rows, hidden), BF)] * 3 + [struct((rows, m * feat // 2), BF)] * 2,
            [tp] + piece + [wg, wu, wd],
            [SM] + [VM] * (m + 3),
            10 * rows * m * feat * hidden,
        )
        parts.append(piece)
        grads.append([d_gate, d_up, active])
        blocks = call(
            functools.partial(pair_sum_kernel, cap),
            [struct((cap, m * feat // 2), BF)] * len(chunk),
            [keep, hop(give, "tp", 1)],
            [VM, VM],
            rows * m * feat,
        )
        for k, block in zip(chunk, blocks):
            back[k] = hop(block, "sp", k) if k else block

    grad_gate, grad_up, grad_down = call(
        functools.partial(weight_kernel, m, len(chunks)),
        [struct(wg.shape, BF), struct(wu.shape, BF), struct(wd.shape, BF)],
        [tp] + [a for piece in parts for a in piece] + [a for g in grads for a in g],
        [SM] + [VM] * (len(chunks) * (m + 3)),
        6 * slots * m * feat * hidden,
    )

    half_width = m * feat // 2
    partial_grad = pl.pallas_call(
        functools.partial(combine_kernel, n, cap),
        out_shape=struct((tok, half_width), BF),
        in_specs=[VM] * (n + 2),
        out_specs=VM,
        scratch_shapes=[pltpu.VMEM((slots, half_width), BF)],
        cost_estimate=pl.CostEstimate(
            flops=2 * slots * tok * half_width, bytes_accessed=slots * half_width * 2, transcendentals=0
        ),
    )(pick, cotangent, *back)
    far = m // 2
    crossed = partial_grad
    bit = far
    while bit > 1:
        pass_on = hop(crossed, "tp", bit)
        width = half_width * bit // m
        flipped = jnp.concatenate(
            [
                pass_on[:, (i ^ (bit >> 1)) * feat : ((i ^ (bit >> 1)) + 1) * feat]
                for i in range(half_width // feat)
            ],
            axis=1,
        )
        crossed = (crossed.astype(F32) + flipped.astype(F32)).astype(BF)
        bit //= 2
    out_grad = crossed
    other_grad = hop(out_grad, "tp", 1)

    grad_gate_pre, local_grad, carry_weight = call(
        functools.partial(recur_kernel, m),
        [struct((tok, channels), BF)] + [struct((tok, channels), F32)] * 2,
        [tp, out_grad, other_grad, out_proj, gate, slope, decay_next],
        [SM] + [VM] * 6,
        2 * tok * m * feat * channels,
    )
    edge = decay_now[0:1] * jnp.concatenate([carry_weight[0:1], local_grad[0:1]], axis=0)
    carried = lax.all_to_all(
        jnp.broadcast_to(edge[None], (n, 2, channels)), "sp", split_axis=0, concat_axis=0, tiled=True
    )
    grad_conv = call(
        functools.partial(final_kernel, n),
        [struct((tok, channels), BF)],
        [sp, local_grad, carry_weight, carried, c1, c2, c3, recur_map, input_map],
        [SM] + [VM] * 8,
        4 * tok * channels * recur_map.shape[1],
    )[0]

    low = (tp[0] & 1) == 0
    quarter = {}
    for q in range(m):
        src = other_grad if q & 1 else out_grad
        quarter[q] = src[:, (q >> 1) * feat : ((q >> 1) + 1) * feat]
    bit = 1
    while bit < m:
        on = (tp[0] & bit) != 0
        quarter = {q: jnp.where(on, quarter[q ^ bit], quarter[q]) for q in range(m)}
        bit *= 2
    half = tok // 2
    side = tp[0] & 1
    full = jnp.concatenate([quarter[q] for q in range(m)], axis=1)
    full = lax.dynamic_slice_in_dim(full, side * half, half, axis=0)
    width = m * feat // n
    slices = full.reshape(half, n, width).transpose(1, 0, 2)
    own = lax.all_to_all(slices, "sp", split_axis=0, concat_axis=0, tiled=True)
    other = hop(own, "tp", 1)
    grad_out_proj = call(
        functools.partial(out_proj_kernel, n),
        [struct((width, channels), F32)],
        [sp, side.reshape(1), own, other, all_mixed],
        [SM, SM, VM, VM, VM],
        2 * n * tok * width * channels,
    )[0]
    return (
        grad_gate[None],
        grad_up[None],
        grad_down[None],
        grad_out_proj,
        grad_conv,
        grad_gate_pre,
    )


def solution(mesh):
    placed = (
        P("sp", "tp"),
        P("sp", "tp"),
        P("sp", None),
        P("sp", None),
        P("sp", "tp"),
        P("sp", "tp"),
        P("sp", "tp"),
        P("sp", "tp"),
        P("sp", "tp"),
        P("tp"),
        P(None, "tp"),
        P("tp", None, None),
        P("tp", None, None),
        P("sp", None, "tp"),
        P("sp", None, "tp"),
        P("sp", "tp", None),
    )
    return jax.shard_map(
        body,
        mesh=mesh,
        in_specs=placed,
        out_specs=(
            P("sp", None, "tp"),
            P("sp", None, "tp"),
            P("sp", "tp", None),
            P("sp", "tp"),
            P("sp", "tp"),
            P("sp", "tp"),
        ),
        check_vma=False,
    )
```

```python
import functools

import jax
import jax.numpy as jnp
from jax import lax
from jax.experimental import pallas as pl
from jax.experimental.pallas import tpu as pltpu
from jax.sharding import PartitionSpec as P


BF = jnp.bfloat16
F32 = jnp.float32
VM = pl.BlockSpec(memory_space=pltpu.VMEM)
ANY = pl.BlockSpec(memory_space=pl.ANY)
HB = pl.BlockSpec(memory_space=pltpu.HBM)


def hop(value, axis, bit):
    count = lax.axis_size(axis)
    return lax.ppermute(value, axis, [(i, i ^ bit) for i in range(count)])


def dot(left, right):
    return jnp.dot(left, right, preferred_element_type=F32)


def dot_nt(left, right):
    return lax.dot_general(left, right, (((1,), (1,)), ((), ())), preferred_element_type=F32)


def dot_tn(left, right):
    return lax.dot_general(left, right, (((0,), (0,)), ((), ())), preferred_element_type=F32)


def call(kernel, outs, ins, specs, flops, scratch=(), limit=8):
    nbytes = sum(a.size * a.dtype.itemsize for a in list(outs) + list(ins))
    return pl.pallas_call(
        kernel,
        out_shape=list(outs),
        in_specs=specs,
        out_specs=[VM] * len(outs),
        scratch_shapes=list(scratch),
        compiler_params=pltpu.CompilerParams(vmem_limit_bytes=limit * 2**20),
        cost_estimate=pl.CostEstimate(flops=flops, bytes_accessed=nbytes, transcendentals=0),
    )(*ins)


def struct(shape, dtype):
    return jax.ShapeDtypeStruct(shape, dtype)


def dispatch_kernel(n, cap, *refs):
    d_ref, first_ref, blocks = refs[4], refs[5], refs[6 : 6 + n]
    held, sems = refs[6 + n : 10 + n], refs[10 + n]
    me = lax.axis_index("sp")
    copies = [pltpu.make_async_copy(refs[i], held[i], sems.at[i]) for i in range(4)]
    for copy in copies:
        copy.start()
    for copy in copies:
        copy.wait()
    ids_ref, w_ref, x_ref, g_ref = held
    tok, feat = x_ref.shape
    ids = ids_ref[...] ^ me
    who = lax.broadcasted_iota(jnp.int32, (n, tok), 0)
    earlier = (
        lax.broadcasted_iota(jnp.int32, (tok, tok), 0)
        < lax.broadcasted_iota(jnp.int32, (tok, tok), 1)
    )
    earlier = jnp.where(earlier, 1.0, 0.0).astype(BF)
    one = [jnp.where(who == ids[k : k + 1, :], 1.0, 0.0) for k in range(2)]
    before = [dot(o.astype(BF), earlier) for o in one]
    before[1] = before[1] + jnp.sum(one[0], axis=1, keepdims=True)
    rank = [jnp.sum(b * o, axis=0, keepdims=True) for b, o in zip(before, one)]
    pos = [ids[k : k + 1, :] * cap + rank[k].astype(jnp.int32) for k in range(2)]
    slot = lax.broadcasted_iota(jnp.int32, (n * cap, tok), 0)
    hit = [slot == p for p in pos]
    weight = jnp.where(hit[0], w_ref[0:1, :], 0.0) + jnp.where(hit[1], w_ref[1:2, :], 0.0)
    weight = jnp.sum(weight, axis=1, keepdims=True)
    pick = jnp.where(hit[0] | hit[1], 1.0, 0.0).astype(BF)
    d_ref[...] = pick
    row = lax.broadcasted_iota(jnp.int32, first_ref.shape, 0)
    first_ref[...] = jnp.where((row == 0) & (me == 0), 1.0, 0.0)
    rows = dot(pick, x_ref[...]).astype(BF)
    cots = (dot(pick, g_ref[...]) * weight).astype(BF)
    for k, block in enumerate(blocks):
        block[:, :feat] = rows[k * cap : (k + 1) * cap]
        block[:, feat:] = cots[k * cap : (k + 1) * cap]


def expert_kernel(m, *refs):
    me = lax.axis_index("tp")
    parts, (wg_ref, wu_ref, wd_ref) = refs[:m], refs[m : m + 3]
    dg_ref, du_ref, act_ref, keep_ref, send_ref = refs[-5:]
    feat = parts[0].shape[1] // 2

    def span(q):
        return pl.ds(pl.multiple_of((me ^ q) * feat, feat), feat)

    pre_gate = pre_up = d_active = 0.0
    for q in range(m):
        rows = parts[q][:, :feat]
        pre_gate += dot(rows, wg_ref[span(q), :])
        pre_up += dot(rows, wu_ref[span(q), :])
        d_active += dot_nt(parts[q][:, feat:], wd_ref[:, span(q)])
    sig = jax.nn.sigmoid(pre_gate)
    gate_act = pre_gate * sig
    act_ref[...] = (gate_act * pre_up).astype(BF)
    d_gate = (d_active * pre_up * sig * (1.0 + pre_gate * (1.0 - sig))).astype(BF)
    d_up = (d_active * gate_act).astype(BF)
    dg_ref[...] = d_gate
    du_ref[...] = d_up
    for q in range(m):
        part = dot_nt(d_gate, wg_ref[span(q), :]) + dot_nt(d_up, wu_ref[span(q), :])
        target = send_ref if q & 1 else keep_ref
        target[:, (q >> 1) * feat : ((q >> 1) + 1) * feat] = part.astype(BF)


def weight_kernel(m, chunks, *refs):
    me = lax.axis_index("tp")
    parts = [refs[h * m : (h + 1) * m] for h in range(chunks)]
    grads = refs[chunks * m : chunks * (m + 3)]
    gg_ref, gu_ref, gd_ref = refs[-3:]
    feat = parts[0][0].shape[1] // 2
    for q in range(m):
        span = pl.ds(pl.multiple_of((me ^ q) * feat, feat), feat)
        gate = up = down = 0.0
        for h in range(chunks):
            rows = parts[h][q][:, :feat]
            gate += dot_tn(rows, grads[3 * h][...])
            up += dot_tn(rows, grads[3 * h + 1][...])
            down += dot_tn(grads[3 * h + 2][...], parts[h][q][:, feat:])
        gg_ref[span, :] = gate.astype(BF)
        gu_ref[span, :] = up.astype(BF)
        gd_ref[:, span] = down.astype(BF)


def join_kernel(*refs):
    rows = refs[0].shape[0]
    for i, ref in enumerate(refs[:-1]):
        refs[-1][i * rows : (i + 1) * rows, :] = ref[...]


def halve_kernel(feat, keep_ref, got_ref, stay_ref, go_ref):
    count = keep_ref.shape[1] // feat
    for i in range(count):
        cols = slice(i * feat, (i + 1) * feat)
        part = keep_ref[:, cols].astype(F32) + got_ref[:, cols].astype(F32)
        at = slice((i >> 1) * feat, ((i >> 1) + 1) * feat)
        target = go_ref if i & 1 else stay_ref
        target[:, at] = part.astype(target.dtype)


def finish_kernel(cap, keep_ref, got_ref, *outs):
    total = (keep_ref[...].astype(F32) + got_ref[...].astype(F32)).astype(BF)
    for k, out in enumerate(outs):
        out[...] = total[k * cap : (k + 1) * cap]


def combine_kernel(n, cap, d_ref, cot_ref, *refs):
    blocks, out_ref, held = refs[:n], refs[-2], refs[-1]
    for k in range(n):
        held[k * cap : (k + 1) * cap, :] = blocks[k][...]
    out_ref[...] = (dot_tn(d_ref[...], held[...]) + cot_ref[...].astype(F32)).astype(BF)


def recur_kernel(n, m, *refs):
    grads, (op_ref, gate_ref, slope_ref, decay_ref) = refs[:m], refs[m : m + 4]
    dgp_ref, local_ref, weight_ref, send_ref, full_ref = refs[m + 4 :]
    me = lax.axis_index("tp")
    tok, channels = decay_ref.shape
    feat = full_ref.shape[2]
    half, width = tok // 2, send_ref.shape[2]
    total = 0.0
    for q in range(m):
        at = me ^ q
        piece = grads[q][...]
        full_ref[at] = piece
        total += dot(piece, op_ref[pl.ds(pl.multiple_of(at * feat, feat), feat), :])
    dgp_ref[...] = (total * slope_ref[...]).astype(BF)
    value = total * gate_ref[...]
    decay = decay_ref[...]
    first = decay[0:1]
    weight = jnp.concatenate([decay[1:], jnp.ones((1, channels), F32)], axis=0)
    step = 1
    while step < tok:
        pad = jnp.zeros((step, channels), F32)
        value = value + weight * jnp.concatenate([value[step:], pad], axis=0)
        weight = weight * jnp.concatenate([weight[step:], pad + 1.0], axis=0)
        step *= 2
    local_ref[...] = value
    weight_ref[...] = weight
    rows = []
    for edge in (first * weight[0:1], first * value[0:1]):
        high = edge.astype(BF).astype(F32)
        for part in (high, edge - high):
            rows += [part[:, i : i + width] for i in range(0, channels, width)]
    spare = send_ref.shape[1] - half - len(rows)
    if spare:
        rows.append(jnp.zeros((spare, width), F32))
    tail = jnp.concatenate(rows, axis=0).astype(BF)
    own = pl.ds(pl.multiple_of((me & 1) * half, half), half)
    for s in range(n):
        at, col = divmod(s * width, feat)
        send_ref[s, :half, :] = full_ref[at, own, col : col + width]
        send_ref[s, half:, :] = tail


def final_kernel(n, half, local_ref, weight_ref, got_ref, c1_ref, c2_ref, c3_ref, rm_ref,
                 im_ref, out_ref):
    me = lax.axis_index("sp")
    channels, width = local_ref.shape[1], got_ref.shape[2]
    per = channels // width

    def lap(i, incoming):
        s = n - 1 - i
        tail = got_ref[s, half:, :].astype(F32)
        part = [
            jnp.concatenate([tail[p * per + i : p * per + i + 1] for i in range(per)], axis=1)
            for p in range(4)
        ]
        longer = (part[2] + part[3]) + (part[0] + part[1]) * incoming
        return jnp.where(s > me, longer, incoming)

    incoming = lax.fori_loop(0, n - 1, lap, jnp.zeros((1, channels), F32), unroll=n <= 8)
    grad = local_ref[...] + weight_ref[...] * incoming
    d_recur = (grad * c1_ref[...]).astype(BF)
    d_input = (grad * c2_ref[...]).astype(BF)
    groups, width = rm_ref.shape[0], rm_ref.shape[1]
    base = grad * c3_ref[...]
    for b in range(groups):
        cols = slice(b * width, (b + 1) * width)
        part = dot_nt(d_recur[:, cols], rm_ref[b]) + dot_nt(d_input[:, cols], im_ref[b])
        out_ref[:, cols] = (base[:, cols] + part).astype(BF)


def out_proj_kernel(n, tok, orders, own_ref, other_ref, *refs):
    pieces, out_ref, held = refs[: len(orders)], refs[-2], refs[-1]
    half = tok // 2
    me, side = lax.axis_index("sp"), lax.axis_index("tp") & 1
    for piece, order in zip(pieces, orders):
        for i, k in enumerate(order):
            held[me ^ k] = piece[i * tok : (i + 1) * tok]
    total = 0.0
    for s in range(n):
        for part, bit in ((own_ref, 0), (other_ref, 1)):
            at = pl.ds(pl.multiple_of((side ^ bit) * half, half), half)
            total += dot_tn(part[s, :half, :], held[s, at, :])
    out_ref[...] = total


def body(
    cotangent,
    mixer_out,
    route_ids,
    route_weights,
    conv_out,
    recur_gate,
    input_gate,
    gate_pre,
    states_before,
    decay_rate,
    out_proj,
    recur_map,
    input_map,
    expert_gate,
    expert_up,
    expert_down,
):
    tok, feat = cotangent.shape
    n, m = lax.axis_size("sp"), lax.axis_size("tp")
    cap = 4 * tok // n
    slots = n * cap
    wg, wu, wd = expert_gate[0], expert_up[0], expert_down[0]
    hidden = wg.shape[1]
    channels = conv_out.shape[1]

    sent = call(
        functools.partial(dispatch_kernel, n, cap),
        [struct((slots, tok), BF), struct((tok, 128), F32)] + [struct((cap, 2 * feat), BF)] * n,
        [route_ids.T, route_weights.T, mixer_out, cotangent],
        [HB] * 4,
        4 * slots * tok * feat,
        scratch=[
            pltpu.VMEM((2, tok), jnp.int32),
            pltpu.VMEM((2, tok), F32),
            pltpu.VMEM((tok, feat), BF),
            pltpu.VMEM((tok, feat), BF),
            pltpu.SemaphoreType.DMA((4,)),
        ],
    )
    pick, first, sent = sent[0], sent[1], sent[2:]
    edges = [0, 1, n // 2, 3 * n // 4, n]
    chunks = [range(a, b) for a, b in zip(edges, edges[1:])]
    got = [sent[0]] + [hop(sent[k], "sp", k) for k in range(1, n)]

    rate = decay_rate[None, :]
    recur_f = recur_gate.astype(F32)
    input_f = input_gate.astype(F32)
    conv_f = conv_out.astype(F32)
    before_f = states_before.astype(F32)
    log_decay = -8.0 * recur_f * rate
    decay_now = jnp.exp(log_decay)
    at_start = first[:, :1] > 0.5
    norm_factor = jnp.where(at_start, 1.0, jnp.sqrt(-jnp.expm1(2.0 * log_decay)))
    norm_slope = jnp.where(at_start, 0.0, -jnp.exp(2.0 * log_decay) / norm_factor)
    drive = input_f * conv_f
    kept = decay_now * before_f
    state = kept + norm_factor * drive
    gate, gelu_back = jax.vjp(jax.nn.gelu, gate_pre.astype(F32))
    slope = gelu_back(state)[0]
    mixed = (state * gate).astype(BF)
    c1 = (kept + norm_slope * drive) * (-8.0 * rate) * recur_f * (1.0 - recur_f)
    c3 = norm_factor * input_f
    c2 = c3 * conv_f * (1.0 - input_f)

    parts, grads, back = [], [], [None] * n
    before = []
    for chunk in chunks:
        rows = len(chunk) * cap
        joined = call(
            join_kernel,
            [struct((rows, 2 * feat), BF)],
            [got[k] for k in chunk],
            [VM] * len(chunk),
            rows * feat,
        )
        here = {0: joined[0]}
        if chunk is chunks[-1]:
            pieces, orders = [mixed, hop(mixed, "sp", n // 2)], [[0], [n // 2]]
        bit = m // 2
        while bit:
            for q in sorted(here):
                here[q | bit] = hop(here[q], "tp", bit)
            bit //= 2
        piece = [here[q] for q in range(m)]
        d_gate, d_up, active, keep, give = call(
            functools.partial(expert_kernel, m),
            [struct((rows, hidden), BF)] * 3 + [struct((rows, m * feat // 2), BF)] * 2,
            piece + [wg, wu, wd] + before,
            [VM] * (m + 3) + [ANY] * len(before),
            10 * rows * m * feat * hidden,
            limit=16,
        )
        before = [d_up]
        parts.append(piece)
        grads.append([d_gate, d_up, active])
        bit = 1
        while 2 * bit < m:
            keep, give = call(
                functools.partial(halve_kernel, feat),
                [struct((rows, keep.shape[1] // 2), t) for t in (F32, BF)],
                [keep, hop(give, "tp", bit)],
                [VM, VM],
                rows * m * feat,
            )
            bit *= 2
        blocks = call(
            functools.partial(finish_kernel, cap),
            [struct((cap, feat), BF)] * len(chunk),
            [keep, hop(give, "tp", bit)],
            [VM, VM],
            rows * feat,
        )
        for k, block in zip(chunk, blocks):
            back[k] = hop(block, "sp", k) if k else block

    bit = n // 4
    while bit:
        stacked = jnp.concatenate(pieces, axis=0)
        order = [k for group in orders for k in group]
        pieces.append(hop(stacked, "sp", bit))
        orders.append([k | bit for k in order])
        bit //= 2

    grad_gate, grad_up, grad_down = call(
        functools.partial(weight_kernel, m, len(chunks)),
        [struct(wg.shape, BF), struct(wu.shape, BF), struct(wd.shape, BF)],
        [a for piece in parts for a in piece] + [a for g in grads for a in g],
        [VM] * (len(chunks) * (m + 3)),
        6 * slots * m * feat * hidden,
        limit=24,
    )

    out_grad = {
        0: call(
            functools.partial(combine_kernel, n, cap),
            [struct((tok, feat), BF)],
            [pick, cotangent, *back],
            [VM] * (n + 2),
            2 * slots * tok * feat,
            scratch=[pltpu.VMEM((slots, feat), BF)],
        )[0]
    }
    bit = m // 2
    while bit:
        for q in sorted(out_grad):
            out_grad[q | bit] = hop(out_grad[q], "tp", bit)
        bit //= 2

    half, width = tok // 2, m * feat // n
    spare = -(-4 * channels // width // 16) * 16
    grad_gate_pre, local_grad, carry_weight, slices = call(
        functools.partial(recur_kernel, n, m),
        [struct((tok, channels), BF)]
        + [struct((tok, channels), F32)] * 2
        + [struct((n, half + spare, width), BF)],
        [*[out_grad[q] for q in range(m)], out_proj, gate, slope, decay_now],
        [VM] * (m + 4),
        2 * tok * m * feat * channels,
        scratch=[pltpu.VMEM((m, tok, feat), BF)],
    )
    own = lax.all_to_all(slices, "sp", split_axis=0, concat_axis=0, tiled=True)
    other = hop(own, "tp", 1)
    grad_conv = call(
        functools.partial(final_kernel, n, half),
        [struct((tok, channels), BF)],
        [local_grad, carry_weight, own, c1, c2, c3, recur_map, input_map],
        [VM] * 8,
        4 * tok * channels * recur_map.shape[1],
    )[0]
    grad_out_proj = call(
        functools.partial(out_proj_kernel, n, tok, orders),
        [struct((width, channels), F32)],
        [own, other, *pieces],
        [VM] * (2 + len(pieces)),
        2 * n * tok * width * channels,
        scratch=[pltpu.VMEM((n, tok, channels), BF)],
        limit=32 if n > 8 else 8,
    )[0]
    return (
        grad_gate[None],
        grad_up[None],
        grad_down[None],
        grad_out_proj,
        grad_conv,
        grad_gate_pre,
    )


def solution(mesh):
    placed = (
        P("sp", "tp"),
        P("sp", "tp"),
        P("sp", None),
        P("sp", None),
        P("sp", "tp"),
        P("sp", "tp"),
        P("sp", "tp"),
        P("sp", "tp"),
        P("sp", "tp"),
        P("tp"),
        P(None, "tp"),
        P("tp", None, None),
        P("tp", None, None),
        P("sp", None, "tp"),
        P("sp", None, "tp"),
        P("sp", "tp", None),
    )

    return jax.shard_map(
        body,
        mesh=mesh,
        in_specs=placed,
        out_specs=(
            P("sp", None, "tp"),
            P("sp", None, "tp"),
            P("sp", "tp", None),
            P("sp", "tp"),
            P("sp", "tp"),
            P("sp", "tp"),
        ),
        check_vma=False,
    )
```

```python
import functools

import jax
import jax.numpy as jnp
from jax import lax
from jax.experimental import pallas as pl
from jax.experimental.pallas import tpu as pltpu
from jax.sharding import PartitionSpec as P


BF = jnp.bfloat16
F32 = jnp.float32
VM = pl.BlockSpec(memory_space=pltpu.VMEM)
ANY = pl.BlockSpec(memory_space=pl.ANY)
HB = pl.BlockSpec(memory_space=pltpu.HBM)


def hop(value, axis, bit):
    count = lax.axis_size(axis)
    return lax.ppermute(value, axis, [(i, i ^ bit) for i in range(count)])


def dot(left, right):
    return jnp.dot(left, right, preferred_element_type=F32)


def dot_nt(left, right):
    return lax.dot_general(left, right, (((1,), (1,)), ((), ())), preferred_element_type=F32)


def dot_tn(left, right):
    return lax.dot_general(left, right, (((0,), (0,)), ((), ())), preferred_element_type=F32)


def call(kernel, outs, ins, specs, flops, scratch=(), limit=8):
    nbytes = sum(a.size * a.dtype.itemsize for a in list(outs) + list(ins))
    return pl.pallas_call(
        kernel,
        out_shape=list(outs),
        in_specs=specs,
        out_specs=[VM] * len(outs),
        scratch_shapes=list(scratch),
        compiler_params=pltpu.CompilerParams(vmem_limit_bytes=limit * 2**20),
        cost_estimate=pl.CostEstimate(flops=flops, bytes_accessed=nbytes, transcendentals=0),
    )(*ins)


def struct(shape, dtype):
    return jax.ShapeDtypeStruct(shape, dtype)


def dispatch_kernel(n, cap, *refs):
    d_ref, first_ref, blocks = refs[4], refs[5], refs[6 : 6 + n]
    held, sems = refs[6 + n : 10 + n], refs[10 + n]
    me = lax.axis_index("sp")
    copies = [pltpu.make_async_copy(refs[i], held[i], sems.at[i]) for i in range(4)]
    for copy in copies:
        copy.start()
    for copy in copies:
        copy.wait()
    ids_ref, w_ref, x_ref, g_ref = held
    tok, feat = x_ref.shape
    ids = ids_ref[...] ^ me
    who = lax.broadcasted_iota(jnp.int32, (n, tok), 0)
    earlier = (
        lax.broadcasted_iota(jnp.int32, (tok, tok), 0)
        < lax.broadcasted_iota(jnp.int32, (tok, tok), 1)
    )
    earlier = jnp.where(earlier, 1.0, 0.0).astype(BF)
    one = [jnp.where(who == ids[k : k + 1, :], 1.0, 0.0) for k in range(2)]
    before = [dot(o.astype(BF), earlier) for o in one]
    before[1] = before[1] + jnp.sum(one[0], axis=1, keepdims=True)
    rank = [jnp.sum(b * o, axis=0, keepdims=True) for b, o in zip(before, one)]
    pos = [ids[k : k + 1, :] * cap + rank[k].astype(jnp.int32) for k in range(2)]
    slot = lax.broadcasted_iota(jnp.int32, (n * cap, tok), 0)
    hit = [slot == p for p in pos]
    weight = jnp.where(hit[0], w_ref[0:1, :], 0.0) + jnp.where(hit[1], w_ref[1:2, :], 0.0)
    weight = jnp.sum(weight, axis=1, keepdims=True)
    pick = jnp.where(hit[0] | hit[1], 1.0, 0.0).astype(BF)
    d_ref[...] = pick
    row = lax.broadcasted_iota(jnp.int32, first_ref.shape, 0)
    first_ref[...] = jnp.where((row == 0) & (me == 0), 1.0, 0.0)
    rows = dot(pick, x_ref[...]).astype(BF)
    cots = (dot(pick, g_ref[...]) * weight).astype(BF)
    for k, block in enumerate(blocks):
        block[:, :feat] = rows[k * cap : (k + 1) * cap]
        block[:, feat:] = cots[k * cap : (k + 1) * cap]


def expert_kernel(m, groups, *refs):
    me = lax.axis_index("tp")
    parts, (wg_ref, wu_ref, wd_ref) = refs[:m], refs[groups * m : groups * m + 3]
    if groups > 1:
        parts, refs = refs[-m:], refs[:-m]
        for q in range(m):
            at = 0
            for g in range(groups):
                piece = refs[g * m + q]
                parts[q][at : at + piece.shape[0], :] = piece[...]
                at += piece.shape[0]
    dg_ref, du_ref, act_ref, keep_ref, send_ref = refs[-5:]
    feat = parts[0].shape[1] // 2

    def span(q):
        return pl.ds(pl.multiple_of((me ^ q) * feat, feat), feat)

    pre_gate = pre_up = d_active = 0.0
    for q in range(m):
        rows = parts[q][:, :feat]
        pre_gate += dot(rows, wg_ref[span(q), :])
        pre_up += dot(rows, wu_ref[span(q), :])
        d_active += dot_nt(parts[q][:, feat:], wd_ref[:, span(q)])
    sig = jax.nn.sigmoid(pre_gate)
    gate_act = pre_gate * sig
    act_ref[...] = (gate_act * pre_up).astype(BF)
    d_gate = (d_active * pre_up * sig * (1.0 + pre_gate * (1.0 - sig))).astype(BF)
    d_up = (d_active * gate_act).astype(BF)
    dg_ref[...] = d_gate
    du_ref[...] = d_up
    for q in range(m):
        part = dot_nt(d_gate, wg_ref[span(q), :]) + dot_nt(d_up, wu_ref[span(q), :])
        target = send_ref if q & 1 else keep_ref
        target[:, (q >> 1) * feat : ((q >> 1) + 1) * feat] = part.astype(BF)


def weight_kernel(m, chunks, *refs):
    me = lax.axis_index("tp")
    parts = [refs[h * m : (h + 1) * m] for h in range(chunks)]
    grads = refs[chunks * m : chunks * (m + 3)]
    gg_ref, gu_ref, gd_ref = refs[-3:]
    feat = parts[0][0].shape[1] // 2
    for q in range(m):
        span = pl.ds(pl.multiple_of((me ^ q) * feat, feat), feat)
        gate = up = down = 0.0
        for h in range(chunks):
            rows = parts[h][q][:, :feat]
            gate += dot_tn(rows, grads[3 * h][...])
            up += dot_tn(rows, grads[3 * h + 1][...])
            down += dot_tn(grads[3 * h + 2][...], parts[h][q][:, feat:])
        gg_ref[span, :] = gate.astype(BF)
        gu_ref[span, :] = up.astype(BF)
        gd_ref[:, span] = down.astype(BF)


def join_kernel(*refs):
    at = 0
    for ref in refs[:-1]:
        refs[-1][at : at + ref.shape[0], :] = ref[...]
        at += ref.shape[0]


def halve_kernel(feat, keep_ref, got_ref, stay_ref, go_ref):
    count = keep_ref.shape[1] // feat
    for i in range(count):
        cols = slice(i * feat, (i + 1) * feat)
        part = keep_ref[:, cols].astype(F32) + got_ref[:, cols].astype(F32)
        at = slice((i >> 1) * feat, ((i >> 1) + 1) * feat)
        target = go_ref if i & 1 else stay_ref
        target[:, at] = part.astype(target.dtype)


def finish_kernel(cap, keep_ref, got_ref, *outs):
    total = (keep_ref[...].astype(F32) + got_ref[...].astype(F32)).astype(BF)
    for k, out in enumerate(outs):
        out[...] = total[k * cap : (k + 1) * cap]


def near_kernel(cap, d_ref, cot_ref, *refs):
    blocks, (stay_ref, go_ref, held) = refs[:-3], refs[-3:]
    feat, rows = cot_ref.shape[1], held.shape[0]
    for k, block in enumerate(blocks):
        held[k * cap : (k + 1) * cap, :] = block[...]
    total = dot_tn(d_ref[:rows, :], held[...])
    for i in range(held.shape[1] // feat):
        part = total[:, i * feat : (i + 1) * feat]
        if i == 0:
            part = part + cot_ref[...].astype(F32)
        at = slice((i >> 1) * feat, ((i >> 1) + 1) * feat)
        target = go_ref if i & 1 else stay_ref
        target[:, at] = part.astype(target.dtype)


def combine_kernel(cap, d_ref, near_ref, got_ref, *refs):
    blocks, (out_ref, held) = refs[:-2], refs[-2:]
    for k, block in enumerate(blocks):
        held[k * cap : (k + 1) * cap, :] = block[...]
    total = dot_tn(d_ref[d_ref.shape[0] - held.shape[0] :, :], held[...])
    out_ref[...] = (total + near_ref[...] + got_ref[...].astype(F32)).astype(BF)


def recur_kernel(n, m, *refs):
    grads, (op_ref, gate_ref, slope_ref, decay_ref) = refs[:m], refs[m : m + 4]
    dgp_ref, local_ref, weight_ref, send_ref, full_ref = refs[m + 4 :]
    me = lax.axis_index("tp")
    tok, channels = decay_ref.shape
    feat = full_ref.shape[2]
    half, width = tok // 2, send_ref.shape[2]
    total = 0.0
    for q in range(m):
        at = me ^ q
        piece = grads[q][...]
        full_ref[at] = piece
        total += dot(piece, op_ref[pl.ds(pl.multiple_of(at * feat, feat), feat), :])
    dgp_ref[...] = (total * slope_ref[...]).astype(BF)
    value = total * gate_ref[...]
    decay = decay_ref[...]
    first = decay[0:1]
    weight = jnp.concatenate([decay[1:], jnp.ones((1, channels), F32)], axis=0)
    step = 1
    while step < tok:
        pad = jnp.zeros((step, channels), F32)
        value = value + weight * jnp.concatenate([value[step:], pad], axis=0)
        weight = weight * jnp.concatenate([weight[step:], pad + 1.0], axis=0)
        step *= 2
    local_ref[...] = value
    weight_ref[...] = weight
    rows = []
    for edge in (first * weight[0:1], first * value[0:1]):
        high = edge.astype(BF).astype(F32)
        for part in (high, edge - high):
            rows += [part[:, i : i + width] for i in range(0, channels, width)]
    spare = send_ref.shape[1] - half - len(rows)
    if spare:
        rows.append(jnp.zeros((spare, width), F32))
    tail = jnp.concatenate(rows, axis=0).astype(BF)
    own = pl.ds(pl.multiple_of((me & 1) * half, half), half)
    for s in range(n):
        at, col = divmod(s * width, feat)
        send_ref[s, :half, :] = full_ref[at, own, col : col + width]
        send_ref[s, half:, :] = tail


def final_kernel(n, half, local_ref, weight_ref, got_ref, c1_ref, c2_ref, c3_ref, rm_ref,
                 im_ref, out_ref):
    me = lax.axis_index("sp")
    channels, width = local_ref.shape[1], got_ref.shape[2]
    per = channels // width

    def lap(i, incoming):
        s = n - 1 - i
        tail = got_ref[s, half:, :].astype(F32)
        part = [
            jnp.concatenate([tail[p * per + i : p * per + i + 1] for i in range(per)], axis=1)
            for p in range(4)
        ]
        longer = (part[2] + part[3]) + (part[0] + part[1]) * incoming
        return jnp.where(s > me, longer, incoming)

    incoming = lax.fori_loop(0, n - 1, lap, jnp.zeros((1, channels), F32), unroll=n <= 8)
    grad = local_ref[...] + weight_ref[...] * incoming
    d_recur = (grad * c1_ref[...]).astype(BF)
    d_input = (grad * c2_ref[...]).astype(BF)
    groups, width = rm_ref.shape[0], rm_ref.shape[1]
    base = grad * c3_ref[...]
    for b in range(groups):
        cols = slice(b * width, (b + 1) * width)
        part = dot_nt(d_recur[:, cols], rm_ref[b]) + dot_nt(d_input[:, cols], im_ref[b])
        out_ref[:, cols] = (base[:, cols] + part).astype(BF)


def out_proj_kernel(n, tok, orders, own_ref, other_ref, *refs):
    pieces, (out_ref, held, grad) = refs[: len(orders)], refs[-3:]
    half = tok // 2
    me, side = lax.axis_index("sp"), lax.axis_index("tp") & 1
    for piece, order in zip(pieces, orders):
        for i, k in enumerate(order):
            held[me ^ k] = piece[i * tok : (i + 1) * tok]
    for s in range(n):
        for part, bit in ((own_ref, 0), (other_ref, 1)):
            at = pl.ds(pl.multiple_of((side ^ bit) * half, half), half)
            grad[s, at, :] = part[s, :half, :]
    flat = grad.shape[0] * grad.shape[1]
    out_ref[...] = dot_tn(
        grad[...].reshape(flat, grad.shape[2]), held[...].reshape(flat, held.shape[2])
    )


def body(
    cotangent,
    mixer_out,
    route_ids,
    route_weights,
    conv_out,
    recur_gate,
    input_gate,
    gate_pre,
    states_before,
    decay_rate,
    out_proj,
    recur_map,
    input_map,
    expert_gate,
    expert_up,
    expert_down,
):
    tok, feat = cotangent.shape
    n, m = lax.axis_size("sp"), lax.axis_size("tp")
    cap = 4 * tok // n
    slots = n * cap
    wg, wu, wd = expert_gate[0], expert_up[0], expert_down[0]
    hidden = wg.shape[1]
    channels = conv_out.shape[1]

    sent = call(
        functools.partial(dispatch_kernel, n, cap),
        [struct((slots, tok), BF), struct((tok, 128), F32)] + [struct((cap, 2 * feat), BF)] * n,
        [route_ids.T, route_weights.T, mixer_out, cotangent],
        [HB] * 4,
        4 * slots * tok * feat,
        scratch=[
            pltpu.VMEM((2, tok), jnp.int32),
            pltpu.VMEM((2, tok), F32),
            pltpu.VMEM((tok, feat), BF),
            pltpu.VMEM((tok, feat), BF),
            pltpu.SemaphoreType.DMA((4,)),
        ],
        limit=60,
    )
    pick, first, sent = sent[0], sent[1], sent[2:]
    edges = [0, n // 4, n // 2, 3 * n // 4, n]
    chunks = [range(a, b) for a, b in zip(edges, edges[1:])]
    got = [sent[0]] + [hop(sent[k], "sp", k) for k in range(1, n)]

    rate = decay_rate[None, :]
    recur_f = recur_gate.astype(F32)
    input_f = input_gate.astype(F32)
    conv_f = conv_out.astype(F32)
    before_f = states_before.astype(F32)
    log_decay = -8.0 * recur_f * rate
    decay_now = jnp.exp(log_decay)
    at_start = first[:, :1] > 0.5
    norm_factor = jnp.where(at_start, 1.0, jnp.sqrt(-jnp.expm1(2.0 * log_decay)))
    norm_slope = jnp.where(at_start, 0.0, -jnp.exp(2.0 * log_decay) / norm_factor)
    drive = input_f * conv_f
    kept = decay_now * before_f
    state = kept + norm_factor * drive
    gate, gelu_back = jax.vjp(jax.nn.gelu, gate_pre.astype(F32))
    slope = gelu_back(state)[0]
    mixed = (state * gate).astype(BF)
    c1 = (kept + norm_slope * drive) * (-8.0 * rate) * recur_f * (1.0 - recur_f)
    c3 = norm_factor * input_f
    c2 = c3 * conv_f * (1.0 - input_f)

    groups, parts, grads, back, before = [], [], [], [], []
    half_width = m * feat // 2
    for h, chunk in enumerate(chunks):
        rows = len(chunk) * cap
        joined = [got[k] for k in chunk]
        if len(chunk) > 1:
            joined = call(
                join_kernel, [struct((rows, 2 * feat), BF)], joined, [VM] * len(chunk), rows * feat
            )
        here = {0: joined[0]}
        if chunk is chunks[-1]:
            pieces = [mixed, hop(mixed, "sp", n // 2)]
        bit = m // 2
        while bit:
            for q in sorted(here):
                here[q | bit] = hop(here[q], "tp", bit)
            bit //= 2
        groups.append([here[q] for q in range(m)])
        if h == 0:
            continue
        merged = []
        if h == 1:
            rows += len(chunks[0]) * cap
            merged = [struct((rows, 2 * feat), BF)] * m
        given = [a for group in groups for a in group]
        made = call(
            functools.partial(expert_kernel, m, len(groups)),
            [struct((rows, hidden), BF)] * 3 + [struct((rows, half_width), BF)] * 2 + merged,
            given + [wg, wu, wd] + before,
            [VM] * (len(given) + 3) + [ANY] * len(before),
            10 * rows * m * feat * hidden,
            limit=16,
        )
        d_gate, d_up, active, keep, give = made[:5]
        before = [d_up]
        parts.append(made[5:] if merged else groups[0])
        groups = []
        grads.append([d_gate, d_up, active])
        if h == 1:
            blocks = call(
                functools.partial(finish_kernel, cap),
                [struct((cap, half_width), BF)] * (n // 2),
                [keep, hop(give, "tp", 1)],
                [VM, VM],
                rows * half_width,
            )
            near = [blocks[0]]
            for k in range(1, n // 2):
                near.append(hop(blocks[k], "sp", k))
            continue
        bit = 1
        while 2 * bit < m:
            keep, give = call(
                functools.partial(halve_kernel, feat),
                [struct((rows, keep.shape[1] // 2), t) for t in (F32, BF)],
                [keep, hop(give, "tp", bit)],
                [VM, VM],
                rows * m * feat,
            )
            bit *= 2
        blocks = call(
            functools.partial(finish_kernel, cap),
            [struct((cap, feat), BF)] * len(chunk),
            [keep, hop(give, "tp", bit)],
            [VM, VM],
            rows * feat,
        )
        back += [hop(block, "sp", k) for k, block in zip(chunk, blocks)]

    stacked = call(
        join_kernel, [struct((2 * tok, channels), BF)], pieces, [VM] * 2, tok * channels
    )[0]
    sources, bit = [(stacked, [0, n // 2])], n // 4
    while bit:
        for source, order in list(sources):
            moved = hop(source, "sp", bit)
            sources.append((moved, [k | bit for k in order]))
        bit //= 2
    pieces = [source for source, _ in sources]
    orders = [order for _, order in sources]

    grad_gate, grad_up, grad_down = call(
        functools.partial(weight_kernel, m, len(parts)),
        [struct(wg.shape, BF), struct(wu.shape, BF), struct(wd.shape, BF)],
        [a for piece in parts for a in piece] + [a for g in grads for a in g],
        [VM] * (len(parts) * (m + 3)),
        6 * slots * m * feat * hidden,
        limit=24,
    )

    near_rows = slots // 2
    stay, go = call(
        functools.partial(near_kernel, cap),
        [struct((tok, half_width // 2), t) for t in (F32, BF)],
        [pick, cotangent, *near],
        [VM] * (n // 2 + 2),
        2 * near_rows * tok * half_width,
        scratch=[pltpu.VMEM((near_rows, half_width), BF)],
    )
    bit = 2
    while 2 * bit < m:
        stay, go = call(
            functools.partial(halve_kernel, feat),
            [struct((tok, stay.shape[1] // 2), t) for t in (F32, BF)],
            [stay, hop(go, "tp", bit)],
            [VM, VM],
            tok * m * feat,
        )
        bit *= 2
    out_grad = {
        0: call(
            functools.partial(combine_kernel, cap),
            [struct((tok, feat), BF)],
            [pick, stay, hop(go, "tp", bit), *back],
            [VM] * (len(back) + 3),
            2 * near_rows * tok * feat,
            scratch=[pltpu.VMEM((slots - near_rows, feat), BF)],
        )[0]
    }
    bit = m // 2
    while bit:
        for q in sorted(out_grad):
            out_grad[q | bit] = hop(out_grad[q], "tp", bit)
        bit //= 2

    half, width = tok // 2, m * feat // n
    spare = -(-4 * channels // width // 16) * 16
    grad_gate_pre, local_grad, carry_weight, slices = call(
        functools.partial(recur_kernel, n, m),
        [struct((tok, channels), BF)]
        + [struct((tok, channels), F32)] * 2
        + [struct((n, half + spare, width), BF)],
        [*[out_grad[q] for q in range(m)], out_proj, gate, slope, decay_now],
        [VM] * (m + 4),
        2 * tok * m * feat * channels,
        scratch=[pltpu.VMEM((m, tok, feat), BF)],
    )
    own = lax.all_to_all(slices, "sp", split_axis=0, concat_axis=0, tiled=True)
    other = hop(own, "tp", 1)
    grad_conv = call(
        functools.partial(final_kernel, n, half),
        [struct((tok, channels), BF)],
        [local_grad, carry_weight, own, c1, c2, c3, recur_map, input_map],
        [VM] * 8,
        4 * tok * channels * recur_map.shape[1],
    )[0]
    grad_out_proj = call(
        functools.partial(out_proj_kernel, n, tok, orders),
        [struct((width, channels), F32)],
        [own, other, *pieces],
        [VM] * (2 + len(pieces)),
        2 * n * tok * width * channels,
        scratch=[pltpu.VMEM((n, tok, channels), BF), pltpu.VMEM((n, tok, width), BF)],
        limit=32 if n > 8 else 8,
    )[0]
    return (
        grad_gate[None],
        grad_up[None],
        grad_down[None],
        grad_out_proj,
        grad_conv,
        grad_gate_pre,
    )


def solution(mesh):
    placed = (
        P("sp", "tp"),
        P("sp", "tp"),
        P("sp", None),
        P("sp", None),
        P("sp", "tp"),
        P("sp", "tp"),
        P("sp", "tp"),
        P("sp", "tp"),
        P("sp", "tp"),
        P("tp"),
        P(None, "tp"),
        P("tp", None, None),
        P("tp", None, None),
        P("sp", None, "tp"),
        P("sp", None, "tp"),
        P("sp", "tp", None),
    )

    return jax.shard_map(
        body,
        mesh=mesh,
        in_specs=placed,
        out_specs=(
            P("sp", None, "tp"),
            P("sp", None, "tp"),
            P("sp", "tp", None),
            P("sp", "tp"),
            P("sp", "tp"),
            P("sp", "tp"),
        ),
        check_vma=False,
    )
```

```python
import functools

import jax
import jax.numpy as jnp
from jax import lax
from jax.experimental import pallas as pl
from jax.experimental.pallas import tpu as pltpu
from jax.sharding import PartitionSpec as P


BF = jnp.bfloat16
F32 = jnp.float32
VM = pl.BlockSpec(memory_space=pltpu.VMEM)
ANY = pl.BlockSpec(memory_space=pl.ANY)
HB = pl.BlockSpec(memory_space=pltpu.HBM)


def hop(value, axis, bit):
    count = lax.axis_size(axis)
    return lax.ppermute(value, axis, [(i, i ^ bit) for i in range(count)])


def dot(left, right):
    return jnp.dot(left, right, preferred_element_type=F32)


def dot_nt(left, right):
    return lax.dot_general(left, right, (((1,), (1,)), ((), ())), preferred_element_type=F32)


def dot_tn(left, right):
    return lax.dot_general(left, right, (((0,), (0,)), ((), ())), preferred_element_type=F32)


def call(kernel, outs, ins, specs, flops, scratch=(), limit=8):
    nbytes = sum(a.size * a.dtype.itemsize for a in list(outs) + list(ins))
    return pl.pallas_call(
        kernel,
        out_shape=list(outs),
        in_specs=specs,
        out_specs=[VM] * len(outs),
        scratch_shapes=list(scratch),
        compiler_params=pltpu.CompilerParams(vmem_limit_bytes=limit * 2**20),
        cost_estimate=pl.CostEstimate(flops=flops, bytes_accessed=nbytes, transcendentals=0),
    )(*ins)


def struct(shape, dtype):
    return jax.ShapeDtypeStruct(shape, dtype)


def dispatch_kernel(n, cap, own, *refs):
    me = lax.axis_index("sp")
    inputs, blocks, slots = refs[:4], refs[4:], n * cap // 2
    if own:
        d_ref, first_ref, blocks, sems = refs[4], refs[5], refs[6:-5], refs[-1]
        copies = [pltpu.make_async_copy(refs[i], refs[i - 5], sems.at[i]) for i in range(4)]
        for copy in copies:
            copy.start()
        for copy in copies:
            copy.wait()
        inputs, slots = refs[-5:-1], n * cap
    ids_ref, w_ref, x_ref, g_ref = inputs
    tok, feat = x_ref.shape
    ids = ids_ref[...] ^ me
    who = lax.broadcasted_iota(jnp.int32, (n, tok), 0)
    earlier = (
        lax.broadcasted_iota(jnp.int32, (tok, tok), 0)
        < lax.broadcasted_iota(jnp.int32, (tok, tok), 1)
    )
    earlier = jnp.where(earlier, 1.0, 0.0).astype(BF)
    one = [jnp.where(who == ids[k : k + 1, :], 1.0, 0.0) for k in range(2)]
    before = [dot(o.astype(BF), earlier) for o in one]
    before[1] = before[1] + jnp.sum(one[0], axis=1, keepdims=True)
    rank = [jnp.sum(b * o, axis=0, keepdims=True) for b, o in zip(before, one)]
    pos = [ids[k : k + 1, :] * cap + rank[k].astype(jnp.int32) for k in range(2)]
    slot = lax.broadcasted_iota(jnp.int32, (slots, tok), 0)
    hit = [slot == p for p in pos]
    weight = jnp.where(hit[0], w_ref[0:1, :], 0.0) + jnp.where(hit[1], w_ref[1:2, :], 0.0)
    weight = jnp.sum(weight, axis=1, keepdims=True)
    pick = jnp.where(hit[0] | hit[1], 1.0, 0.0).astype(BF)
    if own:
        d_ref[...] = pick
        row = lax.broadcasted_iota(jnp.int32, first_ref.shape, 0)
        first_ref[...] = jnp.where((row == 0) & (me == 0), 1.0, 0.0)
        pick, weight = pick[: slots // 2], weight[: slots // 2]
    rows = dot(pick, x_ref[...]).astype(BF)
    cots = (dot(pick, g_ref[...]) * weight).astype(BF)
    for k, block in enumerate(blocks):
        block[:, :feat] = rows[k * cap : (k + 1) * cap]
        block[:, feat:] = cots[k * cap : (k + 1) * cap]


def expert_kernel(m, groups, *refs):
    me = lax.axis_index("tp")
    parts, (wg_ref, wu_ref, wd_ref) = refs[:m], refs[groups * m : groups * m + 3]
    if groups > 1:
        parts, refs = refs[-m:], refs[:-m]
        for q in range(m):
            at = 0
            for g in range(groups):
                piece = refs[g * m + q]
                parts[q][at : at + piece.shape[0], :] = piece[...]
                at += piece.shape[0]
    dg_ref, du_ref, act_ref, keep_ref, send_ref = refs[-5:]
    feat = parts[0].shape[1] // 2

    def span(q):
        return pl.ds(pl.multiple_of((me ^ q) * feat, feat), feat)

    pre_gate = pre_up = d_active = 0.0
    for q in range(m):
        rows = parts[q][:, :feat]
        pre_gate += dot(rows, wg_ref[span(q), :])
        pre_up += dot(rows, wu_ref[span(q), :])
        d_active += dot_nt(parts[q][:, feat:], wd_ref[:, span(q)])
    sig = jax.nn.sigmoid(pre_gate)
    gate_act = pre_gate * sig
    act_ref[...] = (gate_act * pre_up).astype(BF)
    d_gate = (d_active * pre_up * sig * (1.0 + pre_gate * (1.0 - sig))).astype(BF)
    d_up = (d_active * gate_act).astype(BF)
    dg_ref[...] = d_gate
    du_ref[...] = d_up
    for q in range(m):
        part = dot_nt(d_gate, wg_ref[span(q), :]) + dot_nt(d_up, wu_ref[span(q), :])
        target = send_ref if q & 1 else keep_ref
        target[:, (q >> 1) * feat : ((q >> 1) + 1) * feat] = part.astype(BF)


def weight_kernel(m, chunks, *refs):
    me = lax.axis_index("tp")
    parts = [refs[h * m : (h + 1) * m] for h in range(chunks)]
    grads = refs[chunks * m : chunks * (m + 3)]
    gg_ref, gu_ref, gd_ref, rows_ref, both_ref, act_ref = refs[-6:]
    feat, hidden = parts[0][0].shape[1] // 2, gg_ref.shape[1]
    spans, at = [], 0
    for h in range(chunks):
        spans.append(slice(at, at + parts[h][0].shape[0]))
        at = spans[-1].stop
        both_ref[spans[h], :hidden] = grads[3 * h][...]
        both_ref[spans[h], hidden:] = grads[3 * h + 1][...]
        act_ref[spans[h], :] = grads[3 * h + 2][...]
    active = act_ref[...].T
    for q in range(m):
        span = pl.ds(pl.multiple_of((me ^ q) * feat, feat), feat)
        for h in range(chunks):
            rows_ref[spans[h], :] = parts[h][q][...]
        both = dot_tn(rows_ref[:, :feat], both_ref[...]).astype(BF)
        gg_ref[span, :] = both[:, :hidden]
        gu_ref[span, :] = both[:, hidden:]
        gd_ref[:, span] = dot(active, rows_ref[:, feat:]).astype(BF)


def join_kernel(*refs):
    at = 0
    for ref in refs[:-1]:
        refs[-1][at : at + ref.shape[0], :] = ref[...]
        at += ref.shape[0]


def halve_kernel(feat, keep_ref, got_ref, stay_ref, go_ref):
    count = keep_ref.shape[1] // feat
    for i in range(count):
        cols = slice(i * feat, (i + 1) * feat)
        part = keep_ref[:, cols].astype(F32) + got_ref[:, cols].astype(F32)
        at = slice((i >> 1) * feat, ((i >> 1) + 1) * feat)
        target = go_ref if i & 1 else stay_ref
        target[:, at] = part.astype(target.dtype)


def finish_kernel(cap, keep_ref, got_ref, *outs):
    total = (keep_ref[...].astype(F32) + got_ref[...].astype(F32)).astype(BF)
    for k, out in enumerate(outs):
        out[...] = total[k * cap : (k + 1) * cap]


def near_kernel(cap, d_ref, cot_ref, *refs):
    blocks, (stay_ref, go_ref, held) = refs[:-3], refs[-3:]
    feat, rows = cot_ref.shape[1], held.shape[0]
    for k, block in enumerate(blocks):
        held[k * cap : (k + 1) * cap, :] = block[...]
    total = dot_tn(d_ref[:rows, :], held[...])
    for i in range(held.shape[1] // feat):
        part = total[:, i * feat : (i + 1) * feat]
        if i == 0:
            part = part + cot_ref[...].astype(F32)
        at = slice((i >> 1) * feat, ((i >> 1) + 1) * feat)
        target = go_ref if i & 1 else stay_ref
        target[:, at] = part.astype(target.dtype)


def combine_kernel(cap, d_ref, near_ref, got_ref, *refs):
    blocks, (out_ref, held) = refs[:-2], refs[-2:]
    for k, block in enumerate(blocks):
        held[k * cap : (k + 1) * cap, :] = block[...]
    total = dot_tn(d_ref[d_ref.shape[0] - held.shape[0] :, :], held[...])
    out_ref[...] = (total + near_ref[...] + got_ref[...].astype(F32)).astype(BF)


def recur_kernel(n, m, *refs):
    grads, (op_ref, gate_ref, slope_ref, decay_ref) = refs[:m], refs[m : m + 4]
    dgp_ref, local_ref, weight_ref, send_ref, full_ref = refs[m + 4 :]
    me = lax.axis_index("tp")
    tok, channels = decay_ref.shape
    feat = full_ref.shape[2]
    half, width = tok // 2, send_ref.shape[2]
    total = 0.0
    for q in range(m):
        at = me ^ q
        piece = grads[q][...]
        full_ref[at] = piece
        total += dot(piece, op_ref[pl.ds(pl.multiple_of(at * feat, feat), feat), :])
    dgp_ref[...] = (total * slope_ref[...]).astype(BF)
    value = total * gate_ref[...]
    decay = decay_ref[...]
    first = decay[0:1]
    weight = jnp.concatenate([decay[1:], jnp.ones((1, channels), F32)], axis=0)
    step = 1
    while step < tok:
        pad = jnp.zeros((step, channels), F32)
        value = value + weight * jnp.concatenate([value[step:], pad], axis=0)
        weight = weight * jnp.concatenate([weight[step:], pad + 1.0], axis=0)
        step *= 2
    local_ref[...] = value
    weight_ref[...] = weight
    rows = []
    for edge in (first * weight[0:1], first * value[0:1]):
        high = edge.astype(BF).astype(F32)
        for part in (high, edge - high):
            rows += [part[:, i : i + width] for i in range(0, channels, width)]
    spare = send_ref.shape[1] - half - len(rows)
    if spare:
        rows.append(jnp.zeros((spare, width), F32))
    tail = jnp.concatenate(rows, axis=0).astype(BF)
    own = pl.ds(pl.multiple_of((me & 1) * half, half), half)
    for s in range(n):
        at, col = divmod(s * width, feat)
        send_ref[s, :half, :] = full_ref[at, own, col : col + width]
        send_ref[s, half:, :] = tail


def final_kernel(n, half, local_ref, weight_ref, got_ref, c1_ref, c2_ref, c3_ref, rm_ref,
                 im_ref, out_ref):
    me = lax.axis_index("sp")
    channels, width = local_ref.shape[1], got_ref.shape[2]
    per = channels // width

    def lap(i, incoming):
        s = n - 1 - i
        tail = got_ref[s, half:, :].astype(F32)
        part = [
            jnp.concatenate([tail[p * per + i : p * per + i + 1] for i in range(per)], axis=1)
            for p in range(4)
        ]
        longer = (part[2] + part[3]) + (part[0] + part[1]) * incoming
        return jnp.where(s > me, longer, incoming)

    incoming = lax.fori_loop(0, n - 1, lap, jnp.zeros((1, channels), F32), unroll=n <= 8)
    grad = local_ref[...] + weight_ref[...] * incoming
    d_recur = (grad * c1_ref[...]).astype(BF)
    d_input = (grad * c2_ref[...]).astype(BF)
    groups, width = rm_ref.shape[0], rm_ref.shape[1]
    base = grad * c3_ref[...]
    for b in range(groups):
        cols = slice(b * width, (b + 1) * width)
        part = dot_nt(d_recur[:, cols], rm_ref[b]) + dot_nt(d_input[:, cols], im_ref[b])
        out_ref[:, cols] = (base[:, cols] + part).astype(BF)


def out_proj_kernel(n, tok, orders, own_ref, other_ref, *refs):
    pieces, (out_ref, held, grad) = refs[: len(orders)], refs[-3:]
    half = tok // 2
    me, side = lax.axis_index("sp"), lax.axis_index("tp") & 1
    for piece, order in zip(pieces, orders):
        for i, k in enumerate(order):
            held[me ^ k] = piece[i * tok : (i + 1) * tok]
    for s in range(n):
        for part, bit in ((own_ref, 0), (other_ref, 1)):
            at = pl.ds(pl.multiple_of((side ^ bit) * half, half), half)
            grad[s, at, :] = part[s, :half, :]
    flat = grad.shape[0] * grad.shape[1]
    out_ref[...] = dot_tn(
        grad[...].reshape(flat, grad.shape[2]), held[...].reshape(flat, held.shape[2])
    )


def body(
    cotangent,
    mixer_out,
    route_ids,
    route_weights,
    conv_out,
    recur_gate,
    input_gate,
    gate_pre,
    states_before,
    decay_rate,
    out_proj,
    recur_map,
    input_map,
    expert_gate,
    expert_up,
    expert_down,
):
    tok, feat = cotangent.shape
    n, m = lax.axis_size("sp"), lax.axis_size("tp")
    cap = 4 * tok // n
    slots = n * cap
    wg, wu, wd = expert_gate[0], expert_up[0], expert_down[0]
    hidden = wg.shape[1]
    channels = conv_out.shape[1]

    sources = [route_ids.T, route_weights.T, mixer_out, cotangent]
    passed = [hop(source, "sp", n // 2) for source in sources]
    sent = call(
        functools.partial(dispatch_kernel, n, cap, True),
        [struct((slots, tok), BF), struct((tok, 128), F32)]
        + [struct((cap, 2 * feat), BF)] * (n // 2),
        sources,
        [HB] * 4,
        2 * slots * tok * feat,
        scratch=[
            pltpu.VMEM((2, tok), jnp.int32),
            pltpu.VMEM((2, tok), F32),
            pltpu.VMEM((tok, feat), BF),
            pltpu.VMEM((tok, feat), BF),
            pltpu.SemaphoreType.DMA((4,)),
        ],
        limit=60,
    )
    pick, first, sent = sent[0], sent[1], sent[2:]
    relayed = call(
        functools.partial(dispatch_kernel, n, cap, False),
        [struct((cap, 2 * feat), BF)] * (n // 2),
        passed,
        [VM] * 4,
        2 * slots * tok * feat,
    )
    edges = [0, n // 4, n // 2, 3 * n // 4, n]
    chunks = [range(a, b) for a, b in zip(edges, edges[1:])]
    got = []
    for k in range(n):
        block = sent[k] if k < n // 2 else relayed[k - n // 2]
        got.append(hop(block, "sp", k % (n // 2)) if k % (n // 2) else block)

    rate = decay_rate[None, :]
    recur_f = recur_gate.astype(F32)
    input_f = input_gate.astype(F32)
    conv_f = conv_out.astype(F32)
    before_f = states_before.astype(F32)
    log_decay = -8.0 * recur_f * rate
    decay_now = jnp.exp(log_decay)
    at_start = first[:, :1] > 0.5
    norm_factor = jnp.where(at_start, 1.0, jnp.sqrt(-jnp.expm1(2.0 * log_decay)))
    norm_slope = jnp.where(at_start, 0.0, -jnp.exp(2.0 * log_decay) / norm_factor)
    drive = input_f * conv_f
    kept = decay_now * before_f
    state = kept + norm_factor * drive
    gate, gelu_back = jax.vjp(jax.nn.gelu, gate_pre.astype(F32))
    slope = gelu_back(state)[0]
    mixed = (state * gate).astype(BF)
    c1 = (kept + norm_slope * drive) * (-8.0 * rate) * recur_f * (1.0 - recur_f)
    c3 = norm_factor * input_f
    c2 = c3 * conv_f * (1.0 - input_f)

    groups, parts, grads, back, before = [], [], [], [], []
    half_width = m * feat // 2
    for h, chunk in enumerate(chunks):
        rows = len(chunk) * cap
        joined = [got[k] for k in chunk]
        if len(chunk) > 1:
            joined = call(
                join_kernel, [struct((rows, 2 * feat), BF)], joined, [VM] * len(chunk), rows * feat
            )
        here = {0: joined[0]}
        if chunk is chunks[-1]:
            pieces = [mixed, hop(mixed, "sp", n // 2)]
        bit = m // 2
        while bit:
            for q in sorted(here):
                here[q | bit] = hop(here[q], "tp", bit)
            bit //= 2
        groups.append([here[q] for q in range(m)])
        if h == 0:
            continue
        merged = []
        if h == 1:
            rows += len(chunks[0]) * cap
            merged = [struct((rows, 2 * feat), BF)] * m
        given = [a for group in groups for a in group]
        made = call(
            functools.partial(expert_kernel, m, len(groups)),
            [struct((rows, hidden), BF)] * 3 + [struct((rows, half_width), BF)] * 2 + merged,
            given + [wg, wu, wd] + before,
            [VM] * (len(given) + 3) + [ANY] * len(before),
            10 * rows * m * feat * hidden,
            limit=16,
        )
        d_gate, d_up, active, keep, give = made[:5]
        before = [d_up]
        parts.append(made[5:] if merged else groups[0])
        groups = []
        grads.append([d_gate, d_up, active])
        if h == 1:
            blocks = call(
                functools.partial(finish_kernel, cap),
                [struct((cap, half_width), BF)] * (n // 2),
                [keep, hop(give, "tp", 1)],
                [VM, VM],
                rows * half_width,
            )
            near = [blocks[0]]
            for k in range(1, n // 2):
                near.append(hop(blocks[k], "sp", k))
            continue
        bit = 1
        while 2 * bit < m:
            keep, give = call(
                functools.partial(halve_kernel, feat),
                [struct((rows, keep.shape[1] // 2), t) for t in (F32, BF)],
                [keep, hop(give, "tp", bit)],
                [VM, VM],
                rows * m * feat,
            )
            bit *= 2
        blocks = call(
            functools.partial(finish_kernel, cap),
            [struct((cap, feat), BF)] * len(chunk),
            [keep, hop(give, "tp", bit)],
            [VM, VM],
            rows * feat,
        )
        back += [hop(block, "sp", k) for k, block in zip(chunk, blocks)]

    stacked = call(
        join_kernel, [struct((2 * tok, channels), BF)], pieces, [VM] * 2, tok * channels
    )[0]
    sources, bit = [(stacked, [0, n // 2])], n // 4
    while bit:
        for source, order in list(sources):
            moved = hop(source, "sp", bit)
            sources.append((moved, [k | bit for k in order]))
        bit //= 2
    pieces = [source for source, _ in sources]
    orders = [order for _, order in sources]

    grad_gate, grad_up, grad_down = call(
        functools.partial(weight_kernel, m, len(parts)),
        [struct(wg.shape, BF), struct(wu.shape, BF), struct(wd.shape, BF)],
        [a for piece in parts for a in piece] + [a for g in grads for a in g],
        [VM] * (len(parts) * (m + 3)),
        6 * slots * m * feat * hidden,
        scratch=[
            pltpu.VMEM((slots, 2 * feat), BF),
            pltpu.VMEM((slots, 2 * hidden), BF),
            pltpu.VMEM((slots, hidden), BF),
        ],
        limit=16,
    )

    near_rows = slots // 2
    stay, go = call(
        functools.partial(near_kernel, cap),
        [struct((tok, half_width // 2), t) for t in (F32, BF)],
        [pick, cotangent, *near],
        [VM] * (n // 2 + 2),
        2 * near_rows * tok * half_width,
        scratch=[pltpu.VMEM((near_rows, half_width), BF)],
    )
    bit = 2
    while 2 * bit < m:
        stay, go = call(
            functools.partial(halve_kernel, feat),
            [struct((tok, stay.shape[1] // 2), t) for t in (F32, BF)],
            [stay, hop(go, "tp", bit)],
            [VM, VM],
            tok * m * feat,
        )
        bit *= 2
    out_grad = {
        0: call(
            functools.partial(combine_kernel, cap),
            [struct((tok, feat), BF)],
            [pick, stay, hop(go, "tp", bit), *back],
            [VM] * (len(back) + 3),
            2 * near_rows * tok * feat,
            scratch=[pltpu.VMEM((slots - near_rows, feat), BF)],
        )[0]
    }
    bit = m // 2
    while bit:
        for q in sorted(out_grad):
            out_grad[q | bit] = hop(out_grad[q], "tp", bit)
        bit //= 2

    half, width = tok // 2, m * feat // n
    spare = -(-4 * channels // width // 16) * 16
    grad_gate_pre, local_grad, carry_weight, slices = call(
        functools.partial(recur_kernel, n, m),
        [struct((tok, channels), BF)]
        + [struct((tok, channels), F32)] * 2
        + [struct((n, half + spare, width), BF)],
        [*[out_grad[q] for q in range(m)], out_proj, gate, slope, decay_now],
        [VM] * (m + 4),
        2 * tok * m * feat * channels,
        scratch=[pltpu.VMEM((m, tok, feat), BF)],
    )
    own = lax.all_to_all(slices, "sp", split_axis=0, concat_axis=0, tiled=True)
    other = hop(own, "tp", 1)
    grad_conv = call(
        functools.partial(final_kernel, n, half),
        [struct((tok, channels), BF)],
        [local_grad, carry_weight, own, c1, c2, c3, recur_map, input_map],
        [VM] * 8,
        4 * tok * channels * recur_map.shape[1],
    )[0]
    grad_out_proj = call(
        functools.partial(out_proj_kernel, n, tok, orders),
        [struct((width, channels), F32)],
        [own, other, *pieces],
        [VM] * (2 + len(pieces)),
        2 * n * tok * width * channels,
        scratch=[pltpu.VMEM((n, tok, channels), BF), pltpu.VMEM((n, tok, width), BF)],
        limit=32 if n > 8 else 8,
    )[0]
    return (
        grad_gate[None],
        grad_up[None],
        grad_down[None],
        grad_out_proj,
        grad_conv,
        grad_gate_pre,
    )


def solution(mesh):
    placed = (
        P("sp", "tp"),
        P("sp", "tp"),
        P("sp", None),
        P("sp", None),
        P("sp", "tp"),
        P("sp", "tp"),
        P("sp", "tp"),
        P("sp", "tp"),
        P("sp", "tp"),
        P("tp"),
        P(None, "tp"),
        P("tp", None, None),
        P("tp", None, None),
        P("sp", None, "tp"),
        P("sp", None, "tp"),
        P("sp", "tp", None),
    )

    return jax.shard_map(
        body,
        mesh=mesh,
        in_specs=placed,
        out_specs=(
            P("sp", None, "tp"),
            P("sp", None, "tp"),
            P("sp", "tp", None),
            P("sp", "tp"),
            P("sp", "tp"),
            P("sp", "tp"),
        ),
        check_vma=False,
    )
```
